32 devices in a mesh: sp: 8 (over z, y), tp: 4 (over x, core).
Axes of the slice: x: 2, y: 2, z: 4, core: 2. Of those that a mesh axis runs over, the one named last changes fastest.
Arguments:
- tokens: bfloat16 [2048, 4096], P('sp'), may hold values from -6 to 6
- norm_gain: float32 [4096], replicated, may hold values from 0.1 to 1.9
- w_query: bfloat16 [4096, 512], P('sp', 'tp'), may hold values from -0.09375 to 0.09375
- w_key: bfloat16 [4096, 512], P('sp', 'tp'), may hold values from -0.09375 to 0.09375
- w_value: bfloat16 [4096, 1024], P('sp', 'tp'), may hold values from -0.09375 to 0.09375
- w_gates: bfloat16 [4096, 2, 2, 4], P(None, None, None, 'tp'), may hold values from -0.09375 to 0.09375
- input_bias: float32 [2, 4], P(None, 'tp'), may hold values from -2 to 90
- forget_bias: float32 [2, 4], P(None, 'tp'), as said below
- decay_shift: float32 [2, 2048, 4], P(None, 'sp', 'tp'), may hold values from -2.5 to 0
- head_gain: float32 [1024], P('tp'), may hold values from 0.1 to 1.9
- w_conv_b: bfloat16 [4096, 1024], P('sp', 'tp'), may hold values from -0.09375 to 0.09375
- w_conv_c: bfloat16 [4096, 1024], P('sp', 'tp'), may hold values from -0.09375 to 0.09375
- w_conv_in: bfloat16 [4096, 1024], P('sp', 'tp'), may hold values from -0.09375 to 0.09375
- conv_taps: bfloat16 [3, 1024], P(None, 'tp'), may hold values from -3.5 to 3.5
- w_out: bfloat16 [2048, 4096], P('sp', 'tp'), may hold values from -0.125 to 0.125
Outputs:
- mixed_out: bfloat16 [2048, 4096], P('sp', 'tp')
The draws below stay inside these ranges and needn't reach their ends.
Inputs may be any that keep to these rules, and one draw needn't show every extreme that they name: `forget_bias`: at most the natural logarithm of 2048 plus 2.
All inputs are finite; a program needn't handle non-finite values.
Results may differ from the reference program's by a relative error of at most 0.02.
Values may be sent and summed in bfloat16 or wider, within the bound.
A program may use at most 128 MiB of HBM per device.

```python
import jax
import jax.numpy as jnp
from jax import lax

D = 4096
HEADS = 4
DQK = 128
DV = 256
BLOCK = 128
TOK_DEV = 256
BW = 1024
SEQ = 2048


def lasting_heads(key):
    shuffled = jax.random.permutation(jax.random.fold_in(key, 7), 2 * HEADS)
    keep_mask = shuffled < HEADS
    return keep_mask.reshape(2, HEADS)


def forget_values(key):
    lasting_mask = lasting_heads(key)
    quick_bias = jax.random.uniform(jax.random.fold_in(key, 11), (2, HEADS), jnp.float32, 3.5, 4.5)
    lasting = jnp.log(jnp.float32(SEQ)) + 1.5 + jax.random.uniform(jax.random.fold_in(key, 12), (2, HEADS), jnp.float32, -0.5, 0.5)
    return jnp.where(lasting_mask, lasting, quick_bias)


def draw_forget_bias(key, part):
    return forget_values(key)


def draw_decay_shift(key, part):
    decay_speed = jax.nn.softplus(-forget_values(key))
    blocks = SEQ // TOK_DEV
    multiplier = jnp.exp(jax.random.uniform(jax.random.fold_in(key, 13), (2, blocks, HEADS), jnp.float32, 0.0, jnp.log(4.0)))
    multiplier = jnp.repeat(multiplier, TOK_DEV, axis=1)
    locations = jax.random.randint(jax.random.fold_in(key, 14), (3, 2, 1, HEADS), 0, SEQ)
    loss_values = -jnp.log1p(-jax.random.uniform(jax.random.fold_in(key, 15), (3, 2, 1, HEADS), jnp.float32, 0.2, 0.5))
    token_positions = jnp.arange(SEQ, dtype=jnp.int32)[None, None, :, None]
    spike_groups = jnp.sum(jnp.where(token_positions == locations, loss_values, 0.0), axis=0)
    return -(multiplier - 1.0) * decay_speed[:, None, :] - spike_groups


def draw_input_bias(key, part):
    base_values = jax.random.uniform(key, (2, HEADS), jnp.float32, -2.0, 1.0)
    return base_values


def levels(stream_key, extent, pieces, low, top_value):
    loudness, own = 1.0, jax.random.fold_in(stream_key, 6)
    for position, shards_of in pieces:
        heights = jnp.exp(jax.random.uniform(jax.random.fold_in(own, position), (shards_of,), jnp.float32, low / len(pieces), top_value / len(pieces)))
        loudness = loudness * jnp.repeat(heights, extent[position] // shards_of).reshape([-1 if axis == position else 1 for axis in range(len(extent))])
    return loudness


def scatter_about(stream_key, shape, spread, most, split=(), held_as=jnp.bfloat16):
    loudness = levels(stream_key, shape, split, -0.22, 0.18) if split else 1.0
    values = jax.random.normal(stream_key, shape, jnp.float32) * spread * loudness
    return jnp.minimum(jnp.maximum(values, -most), most).astype(held_as)


def setup_inputs(seed: int = 0) -> dict:
    keys = jax.random.split(jax.random.key(seed), 16)
    return {
        "tokens": scatter_about(keys[0], (SEQ, D), 1.0, 6.0, ((0, 8),)),
        "norm_gain": jnp.clip(1.0 + 0.18 * jax.random.normal(keys[1], (D,), jnp.float32), 0.1, 1.9),
        "w_query": scatter_about(keys[2], (D, HEADS * DQK), D ** -0.5, 0.09375, ((0, 8), (1, 4))),
        "w_key": scatter_about(keys[3], (D, HEADS * DQK), D ** -0.5, 0.09375, ((0, 8), (1, 4))),
        "w_value": scatter_about(keys[4], (D, BW), D ** -0.5, 0.09375, ((0, 8), (1, 4))),
        "w_gates": scatter_about(keys[5], (D, 2, 2, HEADS), D ** -0.5, 0.09375, ((3, 4),)),
        "input_bias": draw_input_bias(jax.random.fold_in(keys[15], 71), 0),
        "forget_bias": draw_forget_bias(jax.random.fold_in(keys[15], 71), 0),
        "decay_shift": draw_decay_shift(jax.random.fold_in(keys[15], 71), 0),
        "head_gain": jnp.clip(1.0 + 0.18 * jax.random.normal(keys[9], (BW,), jnp.float32), 0.1, 1.9),
        "w_conv_b": scatter_about(keys[10], (D, BW), D ** -0.5, 0.09375, ((0, 8), (1, 4))),
        "w_conv_c": scatter_about(keys[11], (D, BW), D ** -0.5, 0.09375, ((0, 8), (1, 4))),
        "w_conv_in": scatter_about(keys[12], (D, BW), D ** -0.5, 0.09375, ((0, 8), (1, 4))),
        "conv_taps": scatter_about(keys[13], (3, BW), 3 ** -0.5, 3.5, ((1, 4),)),
        "w_out": scatter_about(keys[14], (2 * BW, D), (2 * BW) ** -0.5, 0.125, ((0, 8), (1, 4))),
    }


EPS = 1e-06
HIGH = lax.Precision.HIGHEST

def row_norm(tokens, norm_gain):
    values = tokens.astype(jnp.float32)
    inverse_rms = lax.rsqrt(lax.optimization_barrier(jnp.mean(values * values, axis=-1, keepdims=True)) + EPS)
    return (values * inverse_rms * norm_gain).astype(jnp.bfloat16)

def project(normed, weight):
    return jnp.dot(normed, weight, preferred_element_type=jnp.float32).astype(jnp.bfloat16)

def to_heads(source, head_count):
    length = source.shape[0]
    return source.astype(jnp.float32).reshape(length, head_count, -1).transpose(1, 0, 2)

def direction_pass(queries, keys_all, values_all, in_gate, log_forget):
    head_count, length = in_gate.shape
    block_count = length // BLOCK

    def blocked(source):
        shaped = source.reshape((head_count, block_count, BLOCK) + source.shape[2:])
        return jnp.moveaxis(shaped, 1, 0)
    lower_mask = jnp.tril(jnp.ones((BLOCK, BLOCK), dtype=bool))

    def advance(carried_state, inputs):
        memory, normer, stable = carried_state
        query_block, key_blk, value_blk, gate_blk, forget_blk = inputs
        cumulative = jnp.cumsum(forget_blk, axis=-1)
        log_weight = jnp.where(lower_mask, cumulative[:, :, None] - cumulative[:, None, :] + gate_blk[:, None, :], -jnp.inf)
        carried = cumulative + stable[:, None]
        running_max = jnp.maximum(carried, lax.optimization_barrier(jnp.max(log_weight, axis=-1)))
        scores = jnp.einsum('htd,hsd->hts', query_block, key_blk, precision=HIGH) * jnp.exp(log_weight - running_max[:, :, None])
        carry_weight = jnp.exp(carried - running_max)
        numerator = jnp.einsum('hts,hsv->htv', scores, value_blk, precision=HIGH) + carry_weight[:, :, None] * jnp.einsum('hvd,htd->htv', memory, query_block, precision=HIGH)
        denominator = lax.optimization_barrier(jnp.sum(scores, axis=-1)) + carry_weight * jnp.einsum('hd,htd->ht', normer, query_block, precision=HIGH)
        output = numerator / jnp.maximum(jnp.abs(denominator), jnp.exp(-running_max))[:, :, None]
        block_total = cumulative[:, -1]
        log_update = block_total[:, None] - cumulative + gate_blk
        new_stable = jnp.maximum(block_total + stable, lax.optimization_barrier(jnp.max(log_update, axis=-1)))
        update = jnp.exp(log_update - new_stable[:, None])
        carry_decay = jnp.exp(block_total + stable - new_stable)
        memory = carry_decay[:, None, None] * memory + jnp.einsum('hsv,hsd->hvd', value_blk * update[:, :, None], key_blk, precision=HIGH)
        normer = carry_decay[:, None] * normer + jnp.einsum('hs,hsd->hd', update, key_blk, precision=HIGH)
        return ((memory, normer, new_stable), output)
    starting_value = (jnp.zeros((head_count, DV, DQK), jnp.float32), jnp.zeros((head_count, DQK), jnp.float32), jnp.full((head_count,), -1e+30, jnp.float32))
    ignored, outputs = lax.scan(advance, starting_value, (blocked(queries), blocked(keys_all), blocked(values_all), blocked(in_gate), blocked(log_forget)))
    return jnp.moveaxis(outputs, 0, 1).reshape(head_count, length, DV)

def flipped(source):
    return jnp.flip(source, axis=1)

def reference(tokens, norm_gain, w_query, w_key, w_value, w_gates, input_bias, forget_bias, decay_shift, head_gain, w_conv_b, w_conv_c, w_conv_in, conv_taps, w_out):
    normed = row_norm(tokens, norm_gain)
    length = normed.shape[0]
    queries = to_heads(project(normed, w_query), HEADS) * DQK ** (-0.5)
    keys_all = to_heads(project(normed, w_key), HEADS)
    values_all = to_heads(project(normed, w_value), HEADS)
    gate_pre = jnp.dot(normed, w_gates.reshape(D, 4 * HEADS), preferred_element_type=jnp.float32).reshape(length, 2, 2, HEADS)
    summed = jnp.zeros((HEADS, length, DV), jnp.float32)
    for direction in range(2):
        in_gate = (gate_pre[:, direction, 0, :] + input_bias[direction]).T
        log_forget = (jax.nn.log_sigmoid(gate_pre[:, direction, 1, :] + forget_bias[direction]) + decay_shift[direction]).T
        if direction == 1:
            result = flipped(direction_pass(flipped(queries), flipped(keys_all), flipped(values_all), flipped(in_gate), flipped(log_forget)))
        else:
            result = direction_pass(queries, keys_all, values_all, in_gate, log_forget)
        summed = summed + result
    inverse_rms = lax.rsqrt(lax.optimization_barrier(jnp.mean(summed * summed, axis=-1, keepdims=True)) + EPS)
    lstm_out = ((summed * inverse_rms).transpose(1, 0, 2) * head_gain.reshape(HEADS, DV)).astype(jnp.bfloat16)
    gate_outer = project(normed, w_conv_b)
    gate_inner = project(normed, w_conv_c)
    conv_input = project(normed, w_conv_in)
    mixed_in = (gate_inner.astype(jnp.float32) * conv_input.astype(jnp.float32)).astype(jnp.bfloat16)
    padded = jnp.pad(mixed_in, ((1, 1), (0, 0))).astype(jnp.float32)
    taps_wide = conv_taps.astype(jnp.float32)
    filtered = taps_wide[0] * padded[:-2] + taps_wide[1] * padded[1:-1] + taps_wide[2] * padded[2:]
    conv_out = (gate_outer.astype(jnp.float32) * filtered).astype(jnp.bfloat16).reshape(length, HEADS, DV)
    joined = jnp.stack([lstm_out, conv_out], axis=2).reshape(length, 2 * HEADS * DV)
    return jnp.dot(joined, w_out, preferred_element_type=jnp.float32).astype(jnp.bfloat16)
```

```python
import functools

import jax
import jax.numpy as jnp
from jax import lax
from jax.experimental import pallas as pl
from jax.experimental.pallas import tpu as pltpu
from jax.sharding import PartitionSpec as P

EPS = 1e-06
HIGH = lax.Precision.HIGHEST
LOWEST = -1e30
F32 = jnp.float32
BF16 = jnp.bfloat16


def dot(a, b, dims, precision=None):
    return lax.dot_general(a, b, (dims, ((), ())), precision=precision, preferred_element_type=F32)


NN = ((1,), (0,))
NT = ((1,), (1,))
TN = ((0,), (0,))


def ring_place(index, n):
    odd = lax.rem(index, 2)
    half = lax.div(index, 2)
    return (1 - odd) * half + odd * (n - 1 - half)


def ring_index(place, n):
    late = lax.div(place, n // 2)
    return (1 - late) * (2 * place) + late * (2 * (n - 1 - place) + 1)


def kernel(
    n,
    t,
    dk,
    dv,
    tokens,
    norm_gain,
    w_own,
    wo_own,
    w_gates,
    gate_bias,
    decay,
    head_gain,
    taps,
    out,
    normed,
    w_all,
    wo_all,
    proj,
    state_out,
    pack_out,
    state_in,
    pack_in,
    carry_c,
    carry_n,
    joined,
    w_ss,
    w_rs,
    wo_ss,
    wo_rs,
    st_ss,
    st_rs,
    pk_ss,
    pk_rs,
    j_ss,
    j_rs,
):
    me = lax.axis_index("sp")
    head = lax.axis_index("tp")
    place = ring_place(me, n)
    right = ring_index(lax.rem(place + 1, n), n)
    left = ring_index(lax.rem(place + n - 1, n), n)
    rows = tokens.shape[0]

    barrier = pltpu.get_barrier_semaphore()

    def greet_sp(o, c):
        pl.semaphore_signal(barrier, inc=1, device_id={"sp": lax.rem(me + o, n)})
        return c

    def greet_tp(o, c):
        pl.semaphore_signal(barrier, inc=1, device_id={"tp": lax.rem(head + o, t)})
        return c

    lax.fori_loop(1, n, greet_sp, 0)
    lax.fori_loop(1, t, greet_tp, 0)
    pl.semaphore_wait(barrier, n + t - 2)

    def hop(own, whole, ss, rs, way, step, first):
        depth, width = own.shape
        half = width // 2
        holder = ring_index(lax.rem(place + (n + step if way else n - step), n), n)
        columns = pl.ds(way * half, half)
        there = whole.at[pl.ds(pl.multiple_of(holder * depth, depth), depth), columns]
        return pltpu.make_async_remote_copy(
            src_ref=own.at[:, columns] if first else there,
            dst_ref=there,
            send_sem=ss.at[way, step],
            recv_sem=rs.at[way, step],
            device_id={"sp": left if way else right},
        )

    def ring_start(*ring):
        for way in range(2):
            hop(*ring, way, 0, True).start()

    def ring_step(step, *ring):
        for way in range(2):
            hop(*ring, way, step - 1, False).wait_recv()
            hop(*ring, way, step, False).start()

    def ring_end(*ring):
        for way in range(2):
            hop(*ring, way, n - 2, False).wait_recv()

        def drain(step, c):
            for way in range(2):
                hop(*ring, way, step, False).wait_send()
            return c

        lax.fori_loop(0, n - 1, drain, 0)

    w_ring = (w_own, w_all, w_ss, w_rs)
    wo_ring = (wo_own, wo_all, wo_ss, wo_rs)
    ring_start(*w_ring)

    depth = w_own.shape[0]
    w_all[pl.ds(pl.multiple_of(me * depth, depth), depth), :] = w_own[...]
    depth_o = wo_own.shape[0]
    wo_all[pl.ds(pl.multiple_of(me * depth_o, depth_o), depth_o), :] = wo_own[...]

    chunk = 32

    def norm_rows(i, c):
        span = pl.ds(pl.multiple_of(i * chunk, chunk), chunk)
        values = tokens[span, :].astype(F32)
        inverse = lax.rsqrt(jnp.mean(values * values, axis=-1, keepdims=True) + EPS)
        normed[span, :] = (values * inverse * norm_gain[...]).astype(BF16)
        return c

    lax.fori_loop(0, rows // chunk, norm_rows, 0)

    gates = dot(w_gates[...], normed[...], NT) + gate_bias[...]
    forget = jnp.minimum(gates, 0.0) - jnp.log1p(jnp.exp(-jnp.abs(gates))) + decay[...]
    row_id = lax.broadcasted_iota(jnp.int32, (rows, rows), 0)
    col_id = lax.broadcasted_iota(jnp.int32, (rows, rows), 1)
    upto = (row_id <= col_id).astype(F32)
    after = (row_id >= col_id).astype(F32)
    sums = (dot(forget, upto, NN, HIGH), dot(forget, after, NN, HIGH))
    gates_t = gates.T
    sums_t = (sums[0].T, sums[1].T)

    lax.fori_loop(1, n - 1, lambda s, c: (ring_step(s, *w_ring), c)[1], 0)
    ring_end(*w_ring)

    ring_start(*wo_ring)
    done = [0]

    def advance():
        if done[0] + 1 < n - 1:
            done[0] += 1
            ring_step(done[0], *wo_ring)

    width = 256

    def project(i, c):
        span = pl.ds(pl.multiple_of(i * width, width), width)
        proj[:, span] = dot(normed[...], w_all[:, span], NN).astype(BF16)
        return c

    lax.fori_loop(0, w_own.shape[1] // width, project, 0)

    query = proj[:, :dk]
    keys = proj[:, dk : 2 * dk]
    values = proj[:, 2 * dk : 2 * dk + dv]
    base = 2 * dk + dv
    bw = (proj.shape[1] - base) // 3
    mixed = (proj[:, base + bw : base + 2 * bw].astype(F32) * proj[:, base + 2 * bw :].astype(F32)).astype(BF16).astype(F32)

    keys_f = keys.astype(F32)
    totals = []
    for d in range(2):
        cum_c = sums_t[d][:, 2 + d : 3 + d]
        in_c = gates_t[:, d : d + 1]
        last = rows - 1 if d == 0 else 0
        total = cum_c[last : last + 1, :]
        update = total - cum_c + in_c
        stable = jnp.max(update, axis=0, keepdims=True)
        weighted = keys_f * jnp.exp(update - stable)
        state_out[d] = dot(weighted.astype(BF16), values, TN).astype(BF16)
        edge = mixed[rows - 1 :, :] if d == 0 else mixed[:1, :]
        wide = pack_out.shape[-1]
        pack_out[d, 0:1, :] = edge
        pack_out[d, 1:2, :dk] = jnp.sum(weighted, axis=0, keepdims=True)
        pack_out[d, 1:2, dk:] = jnp.zeros((1, wide - dk), F32)
        pack_out[d, 2:3, :] = jnp.broadcast_to(total, (1, wide))
        pack_out[d, 3:4, :] = jnp.broadcast_to(stable, (1, wide))
        pack_out[d, 4:, :] = jnp.zeros((4, wide), F32)

    def give(o):
        other = lax.rem(me + o, n)
        d = lax.div(me + o, n)
        ids = {"sp": other}
        return (
            pltpu.make_async_remote_copy(state_out.at[d], state_in.at[me], st_ss.at[o], st_rs.at[me], device_id=ids),
            pltpu.make_async_remote_copy(pack_out.at[d], pack_in.at[me], pk_ss.at[o], pk_rs.at[me], device_id=ids),
        )

    def take(o):
        source = lax.rem(me + o, n)
        ids = {"sp": source}
        return (
            pltpu.make_async_remote_copy(state_out.at[0], state_in.at[source], st_ss.at[o], st_rs.at[source], device_id=ids),
            pltpu.make_async_remote_copy(pack_out.at[0], pack_in.at[source], pk_ss.at[o], pk_rs.at[source], device_id=ids),
        )

    def give_all(o, c):
        for copy in give(o):
            copy.start()
        return c

    def take_all(o, c):
        for copy in take(o):
            copy.wait_recv()
        return c

    def give_end(o, c):
        for copy in give(o):
            copy.wait_send()
        return c

    lax.fori_loop(1, n, give_all, 0)
    advance()

    scale = dk ** (-0.5)
    scores = dot(query, keys, NT) * scale
    local = []
    for d in range(2):
        cum_c = sums_t[d][:, 2 + d : 3 + d]
        cum_r = sums[d][2 + d : 3 + d, :]
        in_r = gates[d : d + 1, :]
        allowed = row_id >= col_id if d == 0 else row_id <= col_id
        log_weight = jnp.where(allowed, cum_c - cum_r + in_r, -jnp.inf)
        peak = jnp.max(log_weight, axis=-1, keepdims=True)
        part = scores * jnp.exp(log_weight - peak)
        num = dot(part, values.astype(F32), NN, HIGH)
        local.append((cum_c, peak, num, jnp.sum(part, axis=-1, keepdims=True)))
        advance()

    lax.fori_loop(1, n, take_all, 0)

    before = pack_in[lax.rem(me + n - 1, n), 0:1, :] * jnp.minimum(me, 1).astype(F32)
    behind = pack_in[lax.rem(me + 1, n), 0:1, :] * jnp.minimum(n - 1 - me, 1).astype(F32)
    pos = lax.broadcasted_iota(jnp.int32, mixed.shape, 0)
    prior = jnp.where(pos == 0, before, pltpu.roll(mixed, 1, 0))
    later = jnp.where(pos == rows - 1, behind, pltpu.roll(mixed, rows - 1, 0))
    taps_f = taps[...].astype(F32)
    filtered = taps_f[0:1] * prior + taps_f[1:2] * mixed + taps_f[2:3] * later
    joined[head, :, dv:] = (proj[:, base : base + bw].astype(F32) * filtered).astype(BF16)

    def share(part, o, source):
        columns = pl.ds(part * dv, dv)
        slot = joined.at[source, :, columns]
        return pltpu.make_async_remote_copy(
            slot,
            slot,
            j_ss.at[part, o],
            j_rs.at[part, source],
            device_id={"tp": lax.rem(head + o, t)},
        )

    for o in range(1, t):
        share(1, o, head).start()
    advance()

    summed = None
    query_f = query.astype(F32) * scale
    for d in range(2):
        carry_c[...] = jnp.zeros_like(carry_c)
        carry_n[...] = jnp.zeros_like(carry_n)

        def join(i, peak_in):
            source = i if d == 0 else n - 1 - i
            total = pack_in[source, 2:3, :]
            stable = pack_in[source, 3:4, :]
            new = jnp.maximum(peak_in + total, stable)
            old_w = jnp.exp(peak_in + total - new)
            new_w = jnp.exp(stable - new)
            carry_c[...] = old_w * carry_c[...] + new_w * state_in[source].astype(F32)
            carry_n[...] = old_w * carry_n[...] + new_w * pack_in[source, 1:2, :]
            return new

        peak_in = lax.fori_loop(0, me if d == 0 else n - 1 - me, join, jnp.full((1, dv), LOWEST, F32))
        cum_c, peak, num, den = local[d]
        carried = cum_c + peak_in[:, :1]
        top = jnp.maximum(carried, peak)
        carry_w = jnp.exp(carried - top)
        own_w = jnp.exp(peak - top)
        num = own_w * num + carry_w * dot(query_f, carry_c[...], NN, HIGH)
        den = own_w * den + carry_w * jnp.sum(query_f * carry_n[:, :dk], axis=-1, keepdims=True)
        result = num / jnp.maximum(jnp.abs(den), jnp.exp(-top))
        summed = result if d == 0 else summed + result
        advance()
    inverse = lax.rsqrt(jnp.mean(summed * summed, axis=-1, keepdims=True) + EPS)
    joined[head, :, :dv] = (summed * inverse * head_gain[...]).astype(BF16)
    for o in range(1, t):
        share(0, o, head).start()

    lax.fori_loop(done[0] + 1, n - 1, lambda s, c: (ring_step(s, *wo_ring), c)[1], 0)
    ring_end(*wo_ring)
    for part in range(2):
        for o in range(1, t):
            share(part, o, lax.rem(head + o, t)).wait_recv()

    span_j = 2 * dv

    def emit(i, c):
        span = pl.ds(pl.multiple_of(i * width, width), width)
        total = dot(joined[0], wo_all[0:span_j, span], NN)
        for j in range(1, t):
            total += dot(joined[j], wo_all[j * span_j : (j + 1) * span_j, span], NN)
        out[:, span] = total.astype(BF16)
        return c

    lax.fori_loop(0, out.shape[1] // width, emit, 0)
    lax.fori_loop(1, n, give_end, 0)
    for part in range(2):
        for o in range(1, t):
            share(part, o, head).wait_send()


def body(
    n,
    t,
    tokens,
    norm_gain,
    w_query,
    w_key,
    w_value,
    w_gates,
    input_bias,
    forget_bias,
    decay_shift,
    head_gain,
    w_conv_b,
    w_conv_c,
    w_conv_in,
    conv_taps,
    w_out,
):
    rows, model = tokens.shape
    dk, dv = w_query.shape[1], w_value.shape[1]
    w_own = jnp.concatenate([w_query, w_key, w_value, w_conv_b, w_conv_c, w_conv_in], axis=1)
    gates = jnp.transpose(w_gates[..., 0], (2, 1, 0)).reshape(4, model)
    gates = jnp.pad(gates, ((0, 4), (0, 0)))
    bias = jnp.concatenate([input_bias, forget_bias, jnp.zeros((4, 1), F32)], axis=0)
    decay = jnp.pad(decay_shift[..., 0], ((2, 4), (0, 0)))
    wide, cols = w_own.shape[1], w_out.shape[1]
    vmem = pl.BlockSpec(memory_space=pltpu.VMEM)
    dma = pltpu.SemaphoreType.DMA
    return pl.pallas_call(
        functools.partial(kernel, n, t, dk, dv),
        out_shape=jax.ShapeDtypeStruct((rows, cols), BF16),
        in_specs=[vmem] * 9,
        out_specs=vmem,
        scratch_shapes=[
            pltpu.VMEM((rows, model), BF16),
            pltpu.VMEM((n * w_own.shape[0], wide), BF16),
            pltpu.VMEM((n * w_out.shape[0], cols), BF16),
            pltpu.VMEM((rows, wide), BF16),
            pltpu.VMEM((2, dk, dv), BF16),
            pltpu.VMEM((2, 8, dv), F32),
            pltpu.VMEM((n, dk, dv), BF16),
            pltpu.VMEM((n, 8, dv), F32),
            pltpu.VMEM((dk, dv), F32),
            pltpu.VMEM((1, dv), F32),
            pltpu.VMEM((t, rows, 2 * dv), BF16),
            dma((2, n - 1)),
            dma((2, n - 1)),
            dma((2, n - 1)),
            dma((2, n - 1)),
            dma((n,)),
            dma((n,)),
            dma((n,)),
            dma((n,)),
            dma((2, t)),
            dma((2, t)),
        ],
        compiler_params=pltpu.CompilerParams(
            collective_id=0, has_side_effects=True, vmem_limit_bytes=60 * 1024 * 1024
        ),
    )(
        tokens,
        norm_gain.reshape(1, model),
        w_own,
        w_out,
        gates,
        bias,
        decay,
        head_gain.reshape(1, dv),
        conv_taps,
    )


def solution(mesh):
    placed = (
        P("sp", None),
        P(),
        P("sp", "tp"),
        P("sp", "tp"),
        P("sp", "tp"),
        P(None, None, None, "tp"),
        P(None, "tp"),
        P(None, "tp"),
        P(None, "sp", "tp"),
        P("tp"),
        P("sp", "tp"),
        P("sp", "tp"),
        P("sp", "tp"),
        P(None, "tp"),
        P("sp", "tp"),
    )
    step = functools.partial(body, mesh.shape["sp"], mesh.shape["tp"])
    return jax.shard_map(step, mesh=mesh, in_specs=placed, out_specs=P("sp", "tp"), check_vma=False)
```

```python
import functools

import jax
import jax.numpy as jnp
from jax import lax
from jax.experimental import pallas as pl
from jax.experimental.pallas import tpu as pltpu
from jax.sharding import PartitionSpec as P

EPS = 1e-06
HIGH = lax.Precision.HIGHEST
LOWEST = -1e30
PIECES = 4
F32 = jnp.float32
BF16 = jnp.bfloat16


def dot(a, b, dims, precision=None):
    return lax.dot_general(a, b, (dims, ((), ())), precision=precision, preferred_element_type=F32)


NN = ((1,), (0,))
NT = ((1,), (1,))
TN = ((0,), (0,))


def ring_place(index, n):
    odd = lax.rem(index, 2)
    half = lax.div(index, 2)
    return (1 - odd) * half + odd * (n - 1 - half)


def ring_index(place, n):
    late = lax.div(place, n // 2)
    return (1 - late) * (2 * place) + late * (2 * (n - 1 - place) + 1)


def pieces(own):
    return max(1, min(PIECES, own.shape[0] // 16))


def kernel(
    n,
    t,
    dk,
    dv,
    tokens,
    norm_gain,
    w_own,
    wo_own,
    w_gates,
    gate_bias,
    decay,
    head_gain,
    taps,
    out,
    normed,
    w_all,
    wo_all,
    proj,
    state_out,
    pack_out,
    state_in,
    pack_in,
    carry_c,
    carry_n,
    joined,
    w_ss,
    w_rs,
    wo_ss,
    wo_rs,
    st_ss,
    st_rs,
    pk_ss,
    pk_rs,
    j_ss,
    j_rs,
):
    me = lax.axis_index("sp")
    head = lax.axis_index("tp")
    place = ring_place(me, n)
    right = ring_index(lax.rem(place + 1, n), n)
    left = ring_index(lax.rem(place + n - 1, n), n)
    rows = tokens.shape[0]

    barrier = pltpu.get_barrier_semaphore()

    def greet_sp(o, c):
        pl.semaphore_signal(barrier, inc=1, device_id={"sp": lax.rem(me + o, n)})
        return c

    def greet_tp(o, c):
        pl.semaphore_signal(barrier, inc=1, device_id={"tp": lax.rem(head + o, t)})
        return c

    lax.fori_loop(1, n, greet_sp, 0)
    lax.fori_loop(1, t, greet_tp, 0)
    pl.semaphore_wait(barrier, n + t - 2)

    def hop(own, whole, ss, rs, way, step, piece, first):
        depth, width = own.shape
        half, tall = width // 2, depth // pieces(own)
        holder = ring_index(lax.rem(place + (n + step if way else n - step), n), n)
        columns = pl.ds(way * half, half)
        there = whole.at[pl.ds(pl.multiple_of(holder * depth + piece * tall, tall), tall), columns]
        turn = step * pieces(own) + piece
        return pltpu.make_async_remote_copy(
            src_ref=own.at[pl.ds(piece * tall, tall), columns] if first else there,
            dst_ref=there,
            send_sem=ss.at[way, turn],
            recv_sem=rs.at[way, turn],
            device_id={"sp": left if way else right},
        )

    def ring_start(*ring):
        for piece in range(pieces(ring[0])):
            for way in range(2):
                hop(*ring, way, 0, piece, True).start()

    def ring_step(step, *ring):
        for piece in range(pieces(ring[0])):
            for way in range(2):
                hop(*ring, way, step - 1, piece, False).wait_recv()
                hop(*ring, way, step, piece, False).start()

    def ring_last(*ring):
        for piece in range(pieces(ring[0])):
            for way in range(2):
                hop(*ring, way, n - 2, piece, False).wait_recv()

    def ring_drain(*ring):
        def drain(step, c):
            for piece in range(pieces(ring[0])):
                for way in range(2):
                    hop(*ring, way, step, piece, False).wait_send()
            return c

        lax.fori_loop(0, n - 1, drain, 0)

    w_ring = (w_own, w_all, w_ss, w_rs)
    wo_ring = (wo_own, wo_all, wo_ss, wo_rs)
    ring_start(*w_ring)

    depth = w_own.shape[0]
    w_all[pl.ds(pl.multiple_of(me * depth, depth), depth), :] = w_own[...]
    depth_o = wo_own.shape[0]
    wo_all[pl.ds(pl.multiple_of(me * depth_o, depth_o), depth_o), :] = wo_own[...]

    chunk = 32

    def norm_rows(i, c):
        span = pl.ds(pl.multiple_of(i * chunk, chunk), chunk)
        values = tokens[span, :].astype(F32)
        inverse = lax.rsqrt(jnp.mean(values * values, axis=-1, keepdims=True) + EPS)
        normed[span, :] = (values * inverse * norm_gain[...]).astype(BF16)
        return c

    lax.fori_loop(0, rows // chunk, norm_rows, 0)

    gates = dot(w_gates[...], normed[...], NT) + gate_bias[...]
    forget = jnp.minimum(gates, 0.0) - jnp.log1p(jnp.exp(-jnp.abs(gates))) + decay[...]
    row_id = lax.broadcasted_iota(jnp.int32, (rows, rows), 0)
    col_id = lax.broadcasted_iota(jnp.int32, (rows, rows), 1)
    upto = (row_id <= col_id).astype(F32)
    after = (row_id >= col_id).astype(F32)
    sums = (dot(forget, upto, NN, HIGH), dot(forget, after, NN, HIGH))
    gates_t = gates.T
    sums_t = (sums[0].T, sums[1].T)

    lax.fori_loop(1, n - 1, lambda s, c: (ring_step(s, *w_ring), c)[1], 0)
    ring_start(*wo_ring)
    ring_last(*w_ring)
    done = [0]

    def advance():
        if done[0] + 1 < n - 1:
            done[0] += 1
            ring_step(done[0], *wo_ring)

    width = 256

    def project(i, c):
        span = pl.ds(pl.multiple_of(i * width, width), width)
        proj[:, span] = dot(normed[...], w_all[:, span], NN).astype(BF16)
        return c

    lax.fori_loop(0, w_own.shape[1] // width, project, 0)

    query = proj[:, :dk]
    keys = proj[:, dk : 2 * dk]
    values = proj[:, 2 * dk : 2 * dk + dv]
    base = 2 * dk + dv
    bw = (proj.shape[1] - base) // 3
    mixed = (proj[:, base + bw : base + 2 * bw].astype(F32) * proj[:, base + 2 * bw :].astype(F32)).astype(BF16).astype(F32)

    keys_f = keys.astype(F32)
    totals = []
    for d in range(2):
        cum_c = sums_t[d][:, 2 + d : 3 + d]
        in_c = gates_t[:, d : d + 1]
        last = rows - 1 if d == 0 else 0
        total = cum_c[last : last + 1, :]
        update = total - cum_c + in_c
        stable = jnp.max(update, axis=0, keepdims=True)
        weighted = keys_f * jnp.exp(update - stable)
        state_out[d] = dot(weighted.astype(BF16), values, TN).astype(BF16)
        edge = mixed[rows - 1 :, :] if d == 0 else mixed[:1, :]
        wide = pack_out.shape[-1]
        pack_out[d, 0:1, :] = edge
        pack_out[d, 1:2, :dk] = jnp.sum(weighted, axis=0, keepdims=True)
        pack_out[d, 1:2, dk:] = jnp.zeros((1, wide - dk), F32)
        pack_out[d, 2:3, :] = jnp.broadcast_to(total, (1, wide))
        pack_out[d, 3:4, :] = jnp.broadcast_to(stable, (1, wide))
        pack_out[d, 4:, :] = jnp.zeros((4, wide), F32)

    def give(o):
        other = lax.rem(me + o, n)
        d = lax.div(me + o, n)
        ids = {"sp": other}
        return (
            pltpu.make_async_remote_copy(state_out.at[d], state_in.at[me], st_ss.at[o], st_rs.at[me], device_id=ids),
            pltpu.make_async_remote_copy(pack_out.at[d], pack_in.at[me], pk_ss.at[o], pk_rs.at[me], device_id=ids),
        )

    def take(o):
        source = lax.rem(me + o, n)
        ids = {"sp": source}
        return (
            pltpu.make_async_remote_copy(state_out.at[0], state_in.at[source], st_ss.at[o], st_rs.at[source], device_id=ids),
            pltpu.make_async_remote_copy(pack_out.at[0], pack_in.at[source], pk_ss.at[o], pk_rs.at[source], device_id=ids),
        )

    def give_all(o, c):
        for copy in give(o):
            copy.start()
        return c

    def take_all(o, c):
        for copy in take(o):
            copy.wait_recv()
        return c

    def give_end(o, c):
        for copy in give(o):
            copy.wait_send()
        return c

    lax.fori_loop(1, n, give_all, 0)
    advance()

    scale = dk ** (-0.5)
    scores = dot(query, keys, NT) * scale
    local = []
    for d in range(2):
        cum_c = sums_t[d][:, 2 + d : 3 + d]
        cum_r = sums[d][2 + d : 3 + d, :]
        in_r = gates[d : d + 1, :]
        allowed = row_id >= col_id if d == 0 else row_id <= col_id
        log_weight = jnp.where(allowed, cum_c - cum_r + in_r, -jnp.inf)
        peak = jnp.max(log_weight, axis=-1, keepdims=True)
        part = scores * jnp.exp(log_weight - peak)
        num = dot(part, values.astype(F32), NN, HIGH)
        local.append((cum_c, peak, num, jnp.sum(part, axis=-1, keepdims=True)))
        advance()

    lax.fori_loop(1, n, take_all, 0)

    before = pack_in[lax.rem(me + n - 1, n), 0:1, :] * jnp.minimum(me, 1).astype(F32)
    behind = pack_in[lax.rem(me + 1, n), 0:1, :] * jnp.minimum(n - 1 - me, 1).astype(F32)
    pos = lax.broadcasted_iota(jnp.int32, mixed.shape, 0)
    prior = jnp.where(pos == 0, before, pltpu.roll(mixed, 1, 0))
    later = jnp.where(pos == rows - 1, behind, pltpu.roll(mixed, rows - 1, 0))
    taps_f = taps[...].astype(F32)
    filtered = taps_f[0:1] * prior + taps_f[1:2] * mixed + taps_f[2:3] * later
    joined[head, :, dv:] = (proj[:, base : base + bw].astype(F32) * filtered).astype(BF16)

    def share(part, o, source):
        columns = pl.ds(part * dv, dv)
        slot = joined.at[source, :, columns]
        return pltpu.make_async_remote_copy(
            slot,
            slot,
            j_ss.at[part, o],
            j_rs.at[part, source],
            device_id={"tp": lax.rem(head + o, t)},
        )

    for o in range(1, t):
        share(1, o, head).start()
    advance()

    summed = None
    query_f = query.astype(F32) * scale
    for d in range(2):
        carry_c[...] = jnp.zeros_like(carry_c)
        carry_n[...] = jnp.zeros_like(carry_n)

        def join(i, peak_in):
            source = i if d == 0 else n - 1 - i
            total = pack_in[source, 2:3, :]
            stable = pack_in[source, 3:4, :]
            new = jnp.maximum(peak_in + total, stable)
            old_w = jnp.exp(peak_in + total - new)
            new_w = jnp.exp(stable - new)
            carry_c[...] = old_w * carry_c[...] + new_w * state_in[source].astype(F32)
            carry_n[...] = old_w * carry_n[...] + new_w * pack_in[source, 1:2, :]
            return new

        peak_in = lax.fori_loop(0, me if d == 0 else n - 1 - me, join, jnp.full((1, dv), LOWEST, F32))
        cum_c, peak, num, den = local[d]
        carried = cum_c + peak_in[:, :1]
        top = jnp.maximum(carried, peak)
        carry_w = jnp.exp(carried - top)
        own_w = jnp.exp(peak - top)
        num = own_w * num + carry_w * dot(query_f, carry_c[...], NN, HIGH)
        den = own_w * den + carry_w * jnp.sum(query_f * carry_n[:, :dk], axis=-1, keepdims=True)
        result = num / jnp.maximum(jnp.abs(den), jnp.exp(-top))
        summed = result if d == 0 else summed + result
        if d == 0:
            advance()
    inverse = lax.rsqrt(jnp.mean(summed * summed, axis=-1, keepdims=True) + EPS)
    joined[head, :, :dv] = (summed * inverse * head_gain[...]).astype(BF16)
    for o in range(1, t):
        share(0, o, head).start()

    lax.fori_loop(done[0] + 1, n - 1, lambda s, c: (ring_step(s, *wo_ring), c)[1], 0)
    ring_last(*wo_ring)
    for part in range(2):
        for o in range(1, t):
            share(part, o, lax.rem(head + o, t)).wait_recv()

    span_j = 2 * dv

    def emit(i, c):
        span = pl.ds(pl.multiple_of(i * width, width), width)
        total = dot(joined[0], wo_all[0:span_j, span], NN)
        for j in range(1, t):
            total += dot(joined[j], wo_all[j * span_j : (j + 1) * span_j, span], NN)
        out[:, span] = total.astype(BF16)
        return c

    lax.fori_loop(0, out.shape[1] // width, emit, 0)
    ring_drain(*w_ring)
    ring_drain(*wo_ring)
    lax.fori_loop(1, n, give_end, 0)
    for part in range(2):
        for o in range(1, t):
            share(part, o, head).wait_send()


def body(
    n,
    t,
    tokens,
    norm_gain,
    w_query,
    w_key,
    w_value,
    w_gates,
    input_bias,
    forget_bias,
    decay_shift,
    head_gain,
    w_conv_b,
    w_conv_c,
    w_conv_in,
    conv_taps,
    w_out,
):
    rows, model = tokens.shape
    dk, dv = w_query.shape[1], w_value.shape[1]
    w_own = jnp.concatenate([w_query, w_key, w_value, w_conv_b, w_conv_c, w_conv_in], axis=1)
    gates = jnp.transpose(w_gates[..., 0], (2, 1, 0)).reshape(4, model)
    gates = jnp.pad(gates, ((0, 4), (0, 0)))
    bias = jnp.concatenate([input_bias, forget_bias, jnp.zeros((4, 1), F32)], axis=0)
    decay = jnp.pad(decay_shift[..., 0], ((2, 4), (0, 0)))
    wide, cols = w_own.shape[1], w_out.shape[1]
    vmem = pl.BlockSpec(memory_space=pltpu.VMEM)
    dma = pltpu.SemaphoreType.DMA
    return pl.pallas_call(
        functools.partial(kernel, n, t, dk, dv),
        out_shape=jax.ShapeDtypeStruct((rows, cols), BF16),
        in_specs=[vmem] * 9,
        out_specs=vmem,
        scratch_shapes=[
            pltpu.VMEM((rows, model), BF16),
            pltpu.VMEM((n * w_own.shape[0], wide), BF16),
            pltpu.VMEM((n * w_out.shape[0], cols), BF16),
            pltpu.VMEM((rows, wide), BF16),
            pltpu.VMEM((2, dk, dv), BF16),
            pltpu.VMEM((2, 8, dv), F32),
            pltpu.VMEM((n, dk, dv), BF16),
            pltpu.VMEM((n, 8, dv), F32),
            pltpu.VMEM((dk, dv), F32),
            pltpu.VMEM((1, dv), F32),
            pltpu.VMEM((t, rows, 2 * dv), BF16),
            dma((2, (n - 1) * pieces(w_own))),
            dma((2, (n - 1) * pieces(w_own))),
            dma((2, (n - 1) * pieces(w_out))),
            dma((2, (n - 1) * pieces(w_out))),
            dma((n,)),
            dma((n,)),
            dma((n,)),
            dma((n,)),
            dma((2, t)),
            dma((2, t)),
        ],
        compiler_params=pltpu.CompilerParams(
            collective_id=0, has_side_effects=True, vmem_limit_bytes=60 * 1024 * 1024
        ),
    )(
        tokens,
        norm_gain.reshape(1, model),
        w_own,
        w_out,
        gates,
        bias,
        decay,
        head_gain.reshape(1, dv),
        conv_taps,
    )


def solution(mesh):
    placed = (
        P("sp", None),
        P(),
        P("sp", "tp"),
        P("sp", "tp"),
        P("sp", "tp"),
        P(None, None, None, "tp"),
        P(None, "tp"),
        P(None, "tp"),
        P(None, "sp", "tp"),
        P("tp"),
        P("sp", "tp"),
        P("sp", "tp"),
        P("sp", "tp"),
        P(None, "tp"),
        P("sp", "tp"),
    )
    step = functools.partial(body, mesh.shape["sp"], mesh.shape["tp"])
    return jax.shard_map(step, mesh=mesh, in_specs=placed, out_specs=P("sp", "tp"), check_vma=False)
```

```python
import functools

import jax
import jax.numpy as jnp
from jax import lax
from jax.experimental import pallas as pl
from jax.experimental.pallas import tpu as pltpu
from jax.sharding import PartitionSpec as P

EPS = 1e-06
HIGH = lax.Precision.HIGHEST
LOWEST = -1e30
PIECES = 4
F32 = jnp.float32
BF16 = jnp.bfloat16


def dot(a, b, dims, precision=None):
    return lax.dot_general(a, b, (dims, ((), ())), precision=precision, preferred_element_type=F32)


NN = ((1,), (0,))
NT = ((1,), (1,))
TN = ((0,), (0,))


def ring_place(index, n):
    odd = lax.rem(index, 2)
    half = lax.div(index, 2)
    return (1 - odd) * half + odd * (n - 1 - half)


def ring_index(place, n):
    late = lax.div(place, n // 2)
    return (1 - late) * (2 * place) + late * (2 * (n - 1 - place) + 1)


def pieces(depth):
    return max(1, min(PIECES, depth // 16))


def kernel(
    n,
    t,
    dk,
    dv,
    tokens,
    norm_gain,
    w_query,
    w_key,
    w_value,
    w_conv_b,
    w_conv_c,
    w_conv_in,
    w_out,
    w_gates,
    input_bias,
    forget_bias,
    decay_shift,
    head_gain,
    taps,
    out,
    normed,
    w_all,
    wo_all,
    proj,
    state_out,
    pack_out,
    state_in,
    pack_in,
    carry_c,
    carry_n,
    joined,
    w_ss,
    w_rs,
    wo_ss,
    wo_rs,
    st_ss,
    st_rs,
    pk_ss,
    pk_rs,
    j_ss,
    j_rs,
    own_sem,
    gate_bias,
    decay,
):
    me = lax.axis_index("sp")
    head = lax.axis_index("tp")
    place = ring_place(me, n)
    right = ring_index(lax.rem(place + 1, n), n)
    left = ring_index(lax.rem(place + n - 1, n), n)
    rows = tokens.shape[0]

    parts = (w_query, w_key, w_value, w_conv_b, w_conv_c, w_conv_in)
    copies = []
    offset = 0
    for part in parts:
        depth, cols = part.shape
        spot = w_all.at[pl.ds(pl.multiple_of(me * depth, depth), depth), pl.ds(offset, cols)]
        copies.append(pltpu.make_async_copy(part, spot, own_sem.at[len(copies)]))
        offset += cols
    depth_o = w_out.shape[0]
    spot = wo_all.at[pl.ds(pl.multiple_of(me * depth_o, depth_o), depth_o), :]
    copies.append(pltpu.make_async_copy(w_out, spot, own_sem.at[len(copies)]))
    for copy in copies:
        copy.start()

    barrier = pltpu.get_barrier_semaphore()

    def greet_sp(o, c):
        pl.semaphore_signal(barrier, inc=1, device_id={"sp": lax.rem(me + o, n)})
        return c

    def greet_tp(o, c):
        pl.semaphore_signal(barrier, inc=1, device_id={"tp": lax.rem(head + o, t)})
        return c

    lax.fori_loop(1, n, greet_sp, 0)
    lax.fori_loop(1, t, greet_tp, 0)
    pl.semaphore_wait(barrier, n + t - 2)

    def hop(depth, whole, ss, rs, way, step, piece):
        width = whole.shape[1]
        half, tall = width // 2, depth // pieces(depth)
        holder = ring_index(lax.rem(place + (n + step if way else n - step), n), n)
        columns = pl.ds(way * half, half)
        there = whole.at[pl.ds(pl.multiple_of(holder * depth + piece * tall, tall), tall), columns]
        turn = step * pieces(depth) + piece
        return pltpu.make_async_remote_copy(
            src_ref=there,
            dst_ref=there,
            send_sem=ss.at[way, turn],
            recv_sem=rs.at[way, turn],
            device_id={"sp": left if way else right},
        )

    def ring_start(*ring):
        for piece in range(pieces(ring[0])):
            for way in range(2):
                hop(*ring, way, 0, piece).start()

    def ring_step(step, *ring):
        for piece in range(pieces(ring[0])):
            for way in range(2):
                hop(*ring, way, step - 1, piece).wait_recv()
                hop(*ring, way, step, piece).start()

    def ring_last(*ring):
        for piece in range(pieces(ring[0])):
            for way in range(2):
                hop(*ring, way, n - 2, piece).wait_recv()

    def ring_drain(*ring):
        def drain(step, c):
            for piece in range(pieces(ring[0])):
                for way in range(2):
                    hop(*ring, way, step, piece).wait_send()
            return c

        lax.fori_loop(0, n - 1, drain, 0)

    w_ring = (w_query.shape[0], w_all, w_ss, w_rs)
    wo_ring = (depth_o, wo_all, wo_ss, wo_rs)
    for copy in copies:
        copy.wait()
    ring_start(*w_ring)

    gate_bias[...] = jnp.zeros_like(gate_bias)
    gate_bias[0:2, :] = input_bias[...]
    gate_bias[2:4, :] = forget_bias[...]
    decay[...] = jnp.zeros_like(decay)
    decay[2:4, :] = decay_shift[...]

    chunk = 32

    def norm_rows(i, c):
        span = pl.ds(pl.multiple_of(i * chunk, chunk), chunk)
        values = tokens[span, :].astype(F32)
        inverse = lax.rsqrt(jnp.mean(values * values, axis=-1, keepdims=True) + EPS)
        normed[span, :] = (values * inverse * norm_gain[...]).astype(BF16)
        return c

    lax.fori_loop(0, rows // chunk, norm_rows, 0)

    gates = dot(w_gates[...], normed[...], NT) + gate_bias[...]
    forget = jnp.minimum(gates, 0.0) - jnp.log1p(jnp.exp(-jnp.abs(gates))) + decay[...]
    row_id = lax.broadcasted_iota(jnp.int32, (rows, rows), 0)
    col_id = lax.broadcasted_iota(jnp.int32, (rows, rows), 1)
    upto = (row_id <= col_id).astype(F32)
    after = (row_id >= col_id).astype(F32)
    sums = (dot(forget, upto, NN, HIGH), dot(forget, after, NN, HIGH))
    gates_t = gates.T
    sums_t = (sums[0].T, sums[1].T)

    lax.fori_loop(1, n - 1, lambda s, c: (ring_step(s, *w_ring), c)[1], 0)
    ring_start(*wo_ring)
    ring_last(*w_ring)
    done = [0]

    def advance():
        if done[0] + 1 < n - 1:
            done[0] += 1
            ring_step(done[0], *wo_ring)

    width = 256

    def project(i, c):
        span = pl.ds(pl.multiple_of(i * width, width), width)
        proj[:, span] = dot(normed[...], w_all[:, span], NN).astype(BF16)
        return c

    lax.fori_loop(0, proj.shape[1] // width, project, 0)

    query = proj[:, :dk]
    keys = proj[:, dk : 2 * dk]
    values = proj[:, 2 * dk : 2 * dk + dv]
    base = 2 * dk + dv
    bw = (proj.shape[1] - base) // 3
    mixed = (proj[:, base + bw : base + 2 * bw].astype(F32) * proj[:, base + 2 * bw :].astype(F32)).astype(BF16).astype(F32)

    keys_f = keys.astype(F32)
    totals = []
    for d in range(2):
        cum_c = sums_t[d][:, 2 + d : 3 + d]
        in_c = gates_t[:, d : d + 1]
        last = rows - 1 if d == 0 else 0
        total = cum_c[last : last + 1, :]
        update = total - cum_c + in_c
        stable = jnp.max(update, axis=0, keepdims=True)
        weighted = keys_f * jnp.exp(update - stable)
        state_out[d] = dot(weighted.astype(BF16), values, TN).astype(BF16)
        edge = mixed[rows - 1 :, :] if d == 0 else mixed[:1, :]
        wide = pack_out.shape[-1]
        pack_out[d, 0:1, :] = edge
        pack_out[d, 1:2, :dk] = jnp.sum(weighted, axis=0, keepdims=True)
        pack_out[d, 1:2, dk:] = jnp.zeros((1, wide - dk), F32)
        pack_out[d, 2:3, :] = jnp.broadcast_to(total, (1, wide))
        pack_out[d, 3:4, :] = jnp.broadcast_to(stable, (1, wide))
        pack_out[d, 4:, :] = jnp.zeros((4, wide), F32)

    def give(o):
        other = lax.rem(me + o, n)
        d = lax.div(me + o, n)
        ids = {"sp": other}
        return (
            pltpu.make_async_remote_copy(state_out.at[d], state_in.at[me], st_ss.at[o], st_rs.at[me], device_id=ids),
            pltpu.make_async_remote_copy(pack_out.at[d], pack_in.at[me], pk_ss.at[o], pk_rs.at[me], device_id=ids),
        )

    def take(o):
        source = lax.rem(me + o, n)
        ids = {"sp": source}
        return (
            pltpu.make_async_remote_copy(state_out.at[0], state_in.at[source], st_ss.at[o], st_rs.at[source], device_id=ids),
            pltpu.make_async_remote_copy(pack_out.at[0], pack_in.at[source], pk_ss.at[o], pk_rs.at[source], device_id=ids),
        )

    def give_all(o, c):
        for copy in give(o):
            copy.start()
        return c

    def take_all(o, c):
        for copy in take(o):
            copy.wait_recv()
        return c

    def give_end(o, c):
        for copy in give(o):
            copy.wait_send()
        return c

    lax.fori_loop(1, n, give_all, 0)
    advance()

    scale = dk ** (-0.5)
    scores = dot(query, keys, NT) * scale
    local = []
    for d in range(2):
        cum_c = sums_t[d][:, 2 + d : 3 + d]
        cum_r = sums[d][2 + d : 3 + d, :]
        in_r = gates[d : d + 1, :]
        allowed = row_id >= col_id if d == 0 else row_id <= col_id
        log_weight = jnp.where(allowed, cum_c - cum_r + in_r, -jnp.inf)
        peak = jnp.max(log_weight, axis=-1, keepdims=True)
        part = scores * jnp.exp(log_weight - peak)
        num = dot(part, values.astype(F32), NN, HIGH)
        local.append((cum_c, peak, num, jnp.sum(part, axis=-1, keepdims=True)))
        advance()

    lax.fori_loop(1, n, take_all, 0)

    before = pack_in[lax.rem(me + n - 1, n), 0:1, :] * jnp.minimum(me, 1).astype(F32)
    behind = pack_in[lax.rem(me + 1, n), 0:1, :] * jnp.minimum(n - 1 - me, 1).astype(F32)
    pos = lax.broadcasted_iota(jnp.int32, mixed.shape, 0)
    prior = jnp.where(pos == 0, before, pltpu.roll(mixed, 1, 0))
    later = jnp.where(pos == rows - 1, behind, pltpu.roll(mixed, rows - 1, 0))
    taps_f = taps[...].astype(F32)
    filtered = taps_f[0:1] * prior + taps_f[1:2] * mixed + taps_f[2:3] * later
    joined[head, :, dv:] = (proj[:, base : base + bw].astype(F32) * filtered).astype(BF16)

    def share(part, o, source):
        columns = pl.ds(part * dv, dv)
        slot = joined.at[source, :, columns]
        return pltpu.make_async_remote_copy(
            slot,
            slot,
            j_ss.at[part, o],
            j_rs.at[part, source],
            device_id={"tp": lax.rem(head + o, t)},
        )

    for o in range(1, t):
        share(1, o, head).start()
    advance()

    summed = None
    query_f = query.astype(F32) * scale
    for d in range(2):
        carry_c[...] = jnp.zeros_like(carry_c)
        carry_n[...] = jnp.zeros_like(carry_n)

        def join(i, peak_in):
            source = i if d == 0 else n - 1 - i
            total = pack_in[source, 2:3, :]
            stable = pack_in[source, 3:4, :]
            new = jnp.maximum(peak_in + total, stable)
            old_w = jnp.exp(peak_in + total - new)
            new_w = jnp.exp(stable - new)
            carry_c[...] = old_w * carry_c[...] + new_w * state_in[source].astype(F32)
            carry_n[...] = old_w * carry_n[...] + new_w * pack_in[source, 1:2, :]
            return new

        peak_in = lax.fori_loop(0, me if d == 0 else n - 1 - me, join, jnp.full((1, dv), LOWEST, F32))
        cum_c, peak, num, den = local[d]
        carried = cum_c + peak_in[:, :1]
        top = jnp.maximum(carried, peak)
        carry_w = jnp.exp(carried - top)
        own_w = jnp.exp(peak - top)
        num = own_w * num + carry_w * dot(query_f, carry_c[...], NN, HIGH)
        den = own_w * den + carry_w * jnp.sum(query_f * carry_n[:, :dk], axis=-1, keepdims=True)
        result = num / jnp.maximum(jnp.abs(den), jnp.exp(-top))
        summed = result if d == 0 else summed + result
        if d == 0:
            advance()
    inverse = lax.rsqrt(jnp.mean(summed * summed, axis=-1, keepdims=True) + EPS)
    joined[head, :, :dv] = (summed * inverse * head_gain[...]).astype(BF16)
    for o in range(1, t):
        share(0, o, head).start()

    lax.fori_loop(done[0] + 1, n - 1, lambda s, c: (ring_step(s, *wo_ring), c)[1], 0)
    ring_last(*wo_ring)
    for part in range(2):
        for o in range(1, t):
            share(part, o, lax.rem(head + o, t)).wait_recv()

    span_j = 2 * dv

    def emit(i, c):
        span = pl.ds(pl.multiple_of(i * width, width), width)
        total = dot(joined[0], wo_all[0:span_j, span], NN)
        for j in range(1, t):
            total += dot(joined[j], wo_all[j * span_j : (j + 1) * span_j, span], NN)
        out[:, span] = total.astype(BF16)
        return c

    lax.fori_loop(0, out.shape[1] // width, emit, 0)
    ring_drain(*w_ring)
    ring_drain(*wo_ring)
    lax.fori_loop(1, n, give_end, 0)
    for part in range(2):
        for o in range(1, t):
            share(part, o, head).wait_send()


def body(
    n,
    t,
    tokens,
    norm_gain,
    w_query,
    w_key,
    w_value,
    w_gates,
    input_bias,
    forget_bias,
    decay_shift,
    head_gain,
    w_conv_b,
    w_conv_c,
    w_conv_in,
    conv_taps,
    w_out,
):
    rows, model = tokens.shape
    dk, dv = w_query.shape[1], w_value.shape[1]
    gates = jnp.transpose(w_gates[..., 0], (2, 1, 0)).reshape(4, model)
    gates = jnp.pad(gates, ((0, 4), (0, 0)))
    depth = w_query.shape[0]
    wide, cols = 2 * dk + dv + 3 * w_conv_b.shape[1], w_out.shape[1]
    hbm = pl.BlockSpec(memory_space=pl.ANY)
    vmem = pl.BlockSpec(memory_space=pltpu.VMEM)
    dma = pltpu.SemaphoreType.DMA
    return pl.pallas_call(
        functools.partial(kernel, n, t, dk, dv),
        out_shape=jax.ShapeDtypeStruct((rows, cols), BF16),
        in_specs=[vmem] * 2 + [hbm] * 7 + [vmem] * 6,
        out_specs=vmem,
        scratch_shapes=[
            pltpu.VMEM((rows, model), BF16),
            pltpu.VMEM((n * depth, wide), BF16),
            pltpu.VMEM((n * w_out.shape[0], cols), BF16),
            pltpu.VMEM((rows, wide), BF16),
            pltpu.VMEM((2, dk, dv), BF16),
            pltpu.VMEM((2, 8, dv), F32),
            pltpu.VMEM((n, dk, dv), BF16),
            pltpu.VMEM((n, 8, dv), F32),
            pltpu.VMEM((dk, dv), F32),
            pltpu.VMEM((1, dv), F32),
            pltpu.VMEM((t, rows, 2 * dv), BF16),
            dma((2, (n - 1) * pieces(depth))),
            dma((2, (n - 1) * pieces(depth))),
            dma((2, (n - 1) * pieces(w_out.shape[0]))),
            dma((2, (n - 1) * pieces(w_out.shape[0]))),
            dma((n,)),
            dma((n,)),
            dma((n,)),
            dma((n,)),
            dma((2, t)),
            dma((2, t)),
            dma((7,)),
            pltpu.VMEM((8, 1), F32),
            pltpu.VMEM((8, rows), F32),
        ],
        compiler_params=pltpu.CompilerParams(
            collective_id=0, has_side_effects=True, vmem_limit_bytes=60 * 1024 * 1024
        ),
    )(
        tokens,
        norm_gain.reshape(1, model),
        w_query,
        w_key,
        w_value,
        w_conv_b,
        w_conv_c,
        w_conv_in,
        w_out,
        gates,
        input_bias,
        forget_bias,
        decay_shift[..., 0],
        head_gain.reshape(1, dv),
        conv_taps,
    )


def solution(mesh):
    placed = (
        P("sp", None),
        P(),
        P("sp", "tp"),
        P("sp", "tp"),
        P("sp", "tp"),
        P(None, None, None, "tp"),
        P(None, "tp"),
        P(None, "tp"),
        P(None, "sp", "tp"),
        P("tp"),
        P("sp", "tp"),
        P("sp", "tp"),
        P("sp", "tp"),
        P(None, "tp"),
        P("sp", "tp"),
    )
    step = functools.partial(body, mesh.shape["sp"], mesh.shape["tp"])
    return jax.shard_map(step, mesh=mesh, in_specs=placed, out_specs=P("sp", "tp"), check_vma=False)
```

```python
import functools

import jax
import jax.numpy as jnp
from jax import lax
from jax.experimental import pallas as pl
from jax.experimental.pallas import tpu as pltpu
from jax.sharding import PartitionSpec as P

EPS = 1e-06
HIGH = lax.Precision.HIGHEST
LOWEST = -1e30
PIECES = 8
F32 = jnp.float32
BF16 = jnp.bfloat16


def dot(a, b, dims, precision=None):
    return lax.dot_general(a, b, (dims, ((), ())), precision=precision, preferred_element_type=F32)


NN = ((1,), (0,))
NT = ((1,), (1,))
TN = ((0,), (0,))


def ring_place(index, n):
    odd = lax.rem(index, 2)
    half = lax.div(index, 2)
    return (1 - odd) * half + odd * (n - 1 - half)


def ring_index(place, n):
    late = lax.div(place, n // 2)
    return (1 - late) * (2 * place) + late * (2 * (n - 1 - place) + 1)


def pieces(depth):
    return max(1, min(PIECES, depth // 16))


def kernel(
    n,
    t,
    dk,
    dv,
    tokens,
    norm_gain,
    w_query,
    w_key,
    w_value,
    w_conv_b,
    w_conv_c,
    w_conv_in,
    w_out,
    w_gates,
    input_bias,
    forget_bias,
    decay_shift,
    head_gain,
    taps,
    out,
    normed,
    w_all,
    wo_all,
    proj,
    state_out,
    pack_out,
    state_in,
    pack_in,
    carry_c,
    carry_n,
    joined,
    w_ss,
    w_rs,
    wo_ss,
    wo_rs,
    st_ss,
    st_rs,
    pk_ss,
    pk_rs,
    j_ss,
    j_rs,
    own_sem,
    gate_bias,
    decay,
):
    me = lax.axis_index("sp")
    head = lax.axis_index("tp")
    place = ring_place(me, n)
    right = ring_index(lax.rem(place + 1, n), n)
    left = ring_index(lax.rem(place + n - 1, n), n)
    rows = tokens.shape[0]

    parts = (w_query, w_key, w_value, w_conv_b, w_conv_c, w_conv_in)
    copies = []
    offset = 0
    for part in parts:
        depth, cols = part.shape
        spot = w_all.at[pl.ds(pl.multiple_of(me * depth, depth), depth), pl.ds(offset, cols)]
        copies.append(pltpu.make_async_copy(part, spot, own_sem.at[len(copies)]))
        offset += cols
    depth_o = w_out.shape[0]
    spot = wo_all.at[pl.ds(pl.multiple_of(me * depth_o, depth_o), depth_o), :]
    copies.append(pltpu.make_async_copy(w_out, spot, own_sem.at[len(copies)]))
    for copy in copies:
        copy.start()

    barrier = pltpu.get_barrier_semaphore()

    def greet_sp(o, c):
        pl.semaphore_signal(barrier, inc=1, device_id={"sp": lax.rem(me + o, n)})
        return c

    def greet_tp(o, c):
        pl.semaphore_signal(barrier, inc=1, device_id={"tp": lax.rem(head + o, t)})
        return c

    lax.fori_loop(1, n, greet_sp, 0)
    lax.fori_loop(1, t, greet_tp, 0)
    pl.semaphore_wait(barrier, n + t - 2)

    def hop(depth, whole, ss, rs, way, step, piece):
        width = whole.shape[1]
        half, tall = width // 2, depth // pieces(depth)
        holder = ring_index(lax.rem(place + (n + step if way else n - step), n), n)
        columns = pl.ds(way * half, half)
        there = whole.at[pl.ds(pl.multiple_of(holder * depth + piece * tall, tall), tall), columns]
        turn = step * pieces(depth) + piece
        return pltpu.make_async_remote_copy(
            src_ref=there,
            dst_ref=there,
            send_sem=ss.at[way, turn],
            recv_sem=rs.at[way, turn],
            device_id={"sp": left if way else right},
        )

    def ring_start(*ring):
        for piece in range(pieces(ring[0])):
            for way in range(2):
                hop(*ring, way, 0, piece).start()

    def ring_step(step, *ring):
        for piece in range(pieces(ring[0])):
            for way in range(2):
                hop(*ring, way, step - 1, piece).wait_recv()
                hop(*ring, way, step, piece).start()

    def ring_last(*ring):
        for piece in range(pieces(ring[0])):
            for way in range(2):
                hop(*ring, way, n - 2, piece).wait_recv()

    def ring_drain(*ring):
        def drain(step, c):
            for piece in range(pieces(ring[0])):
                for way in range(2):
                    hop(*ring, way, step, piece).wait_send()
            return c

        lax.fori_loop(0, n - 1, drain, 0)

    w_ring = (w_query.shape[0], w_all, w_ss, w_rs)
    wo_ring = (depth_o, wo_all, wo_ss, wo_rs)
    for copy in copies:
        copy.wait()
    ring_start(*w_ring)

    gate_bias[...] = jnp.zeros_like(gate_bias)
    gate_bias[0:2, :] = input_bias[...]
    gate_bias[2:4, :] = forget_bias[...]
    decay[...] = jnp.zeros_like(decay)
    decay[2:4, :] = decay_shift[...]

    chunk = 32

    def norm_rows(i, c):
        span = pl.ds(pl.multiple_of(i * chunk, chunk), chunk)
        values = tokens[span, :].astype(F32)
        inverse = lax.rsqrt(jnp.mean(values * values, axis=-1, keepdims=True) + EPS)
        normed[span, :] = (values * inverse * norm_gain[...]).astype(BF16)
        return c

    lax.fori_loop(0, rows // chunk, norm_rows, 0)

    gates = dot(w_gates[...], normed[...], NT) + gate_bias[...]
    forget = jnp.minimum(gates, 0.0) - jnp.log1p(jnp.exp(-jnp.abs(gates))) + decay[...]
    row_id = lax.broadcasted_iota(jnp.int32, (rows, rows), 0)
    col_id = lax.broadcasted_iota(jnp.int32, (rows, rows), 1)
    upto = (row_id <= col_id).astype(F32)
    after = (row_id >= col_id).astype(F32)
    sums = (dot(forget, upto, NN, HIGH), dot(forget, after, NN, HIGH))
    gates_t = gates.T
    sums_t = (sums[0].T, sums[1].T)

    lax.fori_loop(1, n - 1, lambda s, c: (ring_step(s, *w_ring), c)[1], 0)
    ring_start(*wo_ring)
    ring_last(*w_ring)
    done = [0]

    def advance():
        if done[0] + 1 < n - 1:
            done[0] += 1
            ring_step(done[0], *wo_ring)

    width = 256

    def project(i, c):
        span = pl.ds(pl.multiple_of(i * width, width), width)
        proj[:, span] = dot(normed[...], w_all[:, span], NN).astype(BF16)
        return c

    lax.fori_loop(0, proj.shape[1] // width, project, 0)

    query = proj[:, :dk]
    keys = proj[:, dk : 2 * dk]
    values = proj[:, 2 * dk : 2 * dk + dv]
    base = 2 * dk + dv
    bw = (proj.shape[1] - base) // 3
    mixed = (proj[:, base + bw : base + 2 * bw].astype(F32) * proj[:, base + 2 * bw :].astype(F32)).astype(BF16).astype(F32)

    keys_f = keys.astype(F32)
    totals = []
    for d in range(2):
        cum_c = sums_t[d][:, 2 + d : 3 + d]
        in_c = gates_t[:, d : d + 1]
        last = rows - 1 if d == 0 else 0
        total = cum_c[last : last + 1, :]
        update = total - cum_c + in_c
        stable = jnp.max(update, axis=0, keepdims=True)
        weighted = keys_f * jnp.exp(update - stable)
        state_out[d] = dot(weighted.astype(BF16), values, TN).astype(BF16)
        edge = mixed[rows - 1 :, :] if d == 0 else mixed[:1, :]
        wide = pack_out.shape[-1]
        pack_out[d, 0:1, :] = edge
        pack_out[d, 1:2, :dk] = jnp.sum(weighted, axis=0, keepdims=True)
        pack_out[d, 1:2, dk:] = jnp.zeros((1, wide - dk), F32)
        pack_out[d, 2:3, :] = jnp.broadcast_to(total, (1, wide))
        pack_out[d, 3:4, :] = jnp.broadcast_to(stable, (1, wide))
        pack_out[d, 4:, :] = jnp.zeros((4, wide), F32)

    def give(o):
        other = lax.rem(me + o, n)
        d = lax.div(me + o, n)
        ids = {"sp": other}
        return (
            pltpu.make_async_remote_copy(state_out.at[d], state_in.at[me], st_ss.at[o], st_rs.at[me], device_id=ids),
            pltpu.make_async_remote_copy(pack_out.at[d], pack_in.at[me], pk_ss.at[o], pk_rs.at[me], device_id=ids),
        )

    def take(o):
        source = lax.rem(me + o, n)
        ids = {"sp": source}
        return (
            pltpu.make_async_remote_copy(state_out.at[0], state_in.at[source], st_ss.at[o], st_rs.at[source], device_id=ids),
            pltpu.make_async_remote_copy(pack_out.at[0], pack_in.at[source], pk_ss.at[o], pk_rs.at[source], device_id=ids),
        )

    def give_all(o, c):
        for copy in give(o):
            copy.start()
        return c

    def take_all(o, c):
        for copy in take(o):
            copy.wait_recv()
        return c

    def give_end(o, c):
        for copy in give(o):
            copy.wait_send()
        return c

    lax.fori_loop(1, n, give_all, 0)
    advance()

    scale = dk ** (-0.5)
    scores = dot(query, keys, NT) * scale
    local = []
    for d in range(2):
        cum_c = sums_t[d][:, 2 + d : 3 + d]
        cum_r = sums[d][2 + d : 3 + d, :]
        in_r = gates[d : d + 1, :]
        allowed = row_id >= col_id if d == 0 else row_id <= col_id
        log_weight = jnp.where(allowed, cum_c - cum_r + in_r, -jnp.inf)
        peak = jnp.max(log_weight, axis=-1, keepdims=True)
        part = scores * jnp.exp(log_weight - peak)
        num = dot(part, values.astype(F32), NN, HIGH)
        local.append((cum_c, peak, num, jnp.sum(part, axis=-1, keepdims=True)))
        advance()

    lax.fori_loop(1, n, take_all, 0)

    before = pack_in[lax.rem(me + n - 1, n), 0:1, :] * jnp.minimum(me, 1).astype(F32)
    behind = pack_in[lax.rem(me + 1, n), 0:1, :] * jnp.minimum(n - 1 - me, 1).astype(F32)
    pos = lax.broadcasted_iota(jnp.int32, mixed.shape, 0)
    prior = jnp.where(pos == 0, before, pltpu.roll(mixed, 1, 0))
    later = jnp.where(pos == rows - 1, behind, pltpu.roll(mixed, rows - 1, 0))
    taps_f = taps[...].astype(F32)
    filtered = taps_f[0:1] * prior + taps_f[1:2] * mixed + taps_f[2:3] * later
    joined[head, :, dv:] = (proj[:, base : base + bw].astype(F32) * filtered).astype(BF16)

    def share(part, o, source):
        columns = pl.ds(part * dv, dv)
        slot = joined.at[source, :, columns]
        return pltpu.make_async_remote_copy(
            slot,
            slot,
            j_ss.at[part, o],
            j_rs.at[part, source],
            device_id={"tp": lax.rem(head + o, t)},
        )

    for o in range(1, t):
        share(1, o, head).start()
    advance()

    summed = None
    query_f = query.astype(F32) * scale
    for d in range(2):
        carry_c[...] = jnp.zeros_like(carry_c)
        carry_n[...] = jnp.zeros_like(carry_n)

        def join(i, peak_in):
            source = i if d == 0 else n - 1 - i
            total = pack_in[source, 2:3, :]
            stable = pack_in[source, 3:4, :]
            new = jnp.maximum(peak_in + total, stable)
            old_w = jnp.exp(peak_in + total - new)
            new_w = jnp.exp(stable - new)
            carry_c[...] = old_w * carry_c[...] + new_w * state_in[source].astype(F32)
            carry_n[...] = old_w * carry_n[...] + new_w * pack_in[source, 1:2, :]
            return new

        peak_in = lax.fori_loop(0, me if d == 0 else n - 1 - me, join, jnp.full((1, dv), LOWEST, F32))
        cum_c, peak, num, den = local[d]
        carried = cum_c + peak_in[:, :1]
        top = jnp.maximum(carried, peak)
        carry_w = jnp.exp(carried - top)
        own_w = jnp.exp(peak - top)
        num = own_w * num + carry_w * dot(query_f, carry_c[...], NN, HIGH)
        den = own_w * den + carry_w * jnp.sum(query_f * carry_n[:, :dk], axis=-1, keepdims=True)
        result = num / jnp.maximum(jnp.abs(den), jnp.exp(-top))
        summed = result if d == 0 else summed + result
        if d == 0:
            advance()
    inverse = lax.rsqrt(jnp.mean(summed * summed, axis=-1, keepdims=True) + EPS)
    joined[head, :, :dv] = (summed * inverse * head_gain[...]).astype(BF16)
    for o in range(1, t):
        share(0, o, head).start()

    lax.fori_loop(done[0] + 1, n - 1, lambda s, c: (ring_step(s, *wo_ring), c)[1], 0)
    ring_last(*wo_ring)
    for part in range(2):
        for o in range(1, t):
            share(part, o, lax.rem(head + o, t)).wait_recv()

    span_j = 2 * dv

    def emit(i, c):
        span = pl.ds(pl.multiple_of(i * width, width), width)
        total = dot(joined[0], wo_all[0:span_j, span], NN)
        for j in range(1, t):
            total += dot(joined[j], wo_all[j * span_j : (j + 1) * span_j, span], NN)
        out[:, span] = total.astype(BF16)
        return c

    lax.fori_loop(0, out.shape[1] // width, emit, 0)
    ring_drain(*w_ring)
    ring_drain(*wo_ring)
    lax.fori_loop(1, n, give_end, 0)
    for part in range(2):
        for o in range(1, t):
            share(part, o, head).wait_send()


def body(
    n,
    t,
    tokens,
    norm_gain,
    w_query,
    w_key,
    w_value,
    w_gates,
    input_bias,
    forget_bias,
    decay_shift,
    head_gain,
    w_conv_b,
    w_conv_c,
    w_conv_in,
    conv_taps,
    w_out,
):
    rows, model = tokens.shape
    dk, dv = w_query.shape[1], w_value.shape[1]
    gates = jnp.transpose(w_gates[..., 0], (2, 1, 0)).reshape(4, model)
    gates = jnp.pad(gates, ((0, 4), (0, 0)))
    depth = w_query.shape[0]
    wide, cols = 2 * dk + dv + 3 * w_conv_b.shape[1], w_out.shape[1]
    hbm = pl.BlockSpec(memory_space=pl.ANY)
    vmem = pl.BlockSpec(memory_space=pltpu.VMEM)
    dma = pltpu.SemaphoreType.DMA
    return pl.pallas_call(
        functools.partial(kernel, n, t, dk, dv),
        out_shape=jax.ShapeDtypeStruct((rows, cols), BF16),
        in_specs=[vmem] * 2 + [hbm] * 7 + [vmem] * 6,
        out_specs=vmem,
        scratch_shapes=[
            pltpu.VMEM((rows, model), BF16),
            pltpu.VMEM((n * depth, wide), BF16),
            pltpu.VMEM((n * w_out.shape[0], cols), BF16),
            pltpu.VMEM((rows, wide), BF16),
            pltpu.VMEM((2, dk, dv), BF16),
            pltpu.VMEM((2, 8, dv), F32),
            pltpu.VMEM((n, dk, dv), BF16),
            pltpu.VMEM((n, 8, dv), F32),
            pltpu.VMEM((dk, dv), F32),
            pltpu.VMEM((1, dv), F32),
            pltpu.VMEM((t, rows, 2 * dv), BF16),
            dma((2, (n - 1) * pieces(depth))),
            dma((2, (n - 1) * pieces(depth))),
            dma((2, (n - 1) * pieces(w_out.shape[0]))),
            dma((2, (n - 1) * pieces(w_out.shape[0]))),
            dma((n,)),
            dma((n,)),
            dma((n,)),
            dma((n,)),
            dma((2, t)),
            dma((2, t)),
            dma((7,)),
            pltpu.VMEM((8, 1), F32),
            pltpu.VMEM((8, rows), F32),
        ],
        compiler_params=pltpu.CompilerParams(
            collective_id=0, has_side_effects=True, vmem_limit_bytes=60 * 1024 * 1024
        ),
    )(
        tokens,
        norm_gain.reshape(1, model),
        w_query,
        w_key,
        w_value,
        w_conv_b,
        w_conv_c,
        w_conv_in,
        w_out,
        gates,
        input_bias,
        forget_bias,
        decay_shift[..., 0],
        head_gain.reshape(1, dv),
        conv_taps,
    )


def solution(mesh):
    placed = (
        P("sp", None),
        P(),
        P("sp", "tp"),
        P("sp", "tp"),
        P("sp", "tp"),
        P(None, None, None, "tp"),
        P(None, "tp"),
        P(None, "tp"),
        P(None, "sp", "tp"),
        P("tp"),
        P("sp", "tp"),
        P("sp", "tp"),
        P("sp", "tp"),
        P(None, "tp"),
        P("sp", "tp"),
    )
    step = functools.partial(body, mesh.shape["sp"], mesh.shape["tp"])
    return jax.shard_map(step, mesh=mesh, in_specs=placed, out_specs=P("sp", "tp"), check_vma=False)
```
